32 devices in a mesh: ep: 8 (over z, core), tp: 4 (over y, x).
Axes of the slice: x: 2, y: 2, z: 4, core: 2. Of those that a mesh axis runs over, the one named last changes fastest.
Arguments:
- conv_input: bfloat16 [1024, 16384], P('tp', 'ep'), may hold values from -6 to 6
- out_gate: bfloat16 [1024, 16384], P('tp', 'ep'), may hold values from -6 to 6
- in_gate: bfloat16 [1024, 16384], P('tp', 'ep'), may hold values from -6 to 6
- conv_taps: float32 [3, 1024], replicated, may hold values from -3.5 to 3.5
- mixer_proj: bfloat16 [1024, 2048], P(None, 'tp'), may hold values from -0.1875 to 0.1875
- token_rows: bfloat16 [2048, 2048], P('ep', 'tp'), may hold values from -4000 to 4000
- routes: int32 [2048, 2], P('ep'), may hold values from 0 to 7, as said below
- route_weights: float32 [2048, 2], P('ep'), may hold values from 0.3 to 1
- expert_gate: bfloat16 [8, 2048, 4096], P('ep', None, 'tp'), may hold values from -0.125 to 0.125
- expert_up: bfloat16 [8, 2048, 4096], P('ep', None, 'tp'), may hold values from -0.125 to 0.125
- expert_down: bfloat16 [8, 4096, 2048], P('ep', 'tp'), may hold values from -0.125 to 0.125
Outputs:
- mixed_out: bfloat16 [16384, 2048], P('ep', 'tp')
- expert_out: bfloat16 [2048, 2048], P('ep', 'tp')
The draws below stay inside these ranges and needn't reach their ends.
Inputs may be any that keep to these rules, and one draw needn't show every extreme that they name: `routes`: in each aligned block of 256 rows, no expert is named more than 128 times and one expert, the same in every block, exactly 128 times; the two experts of a row differ.
All inputs are finite; a program needn't handle non-finite values.
Results may differ from the reference program's by a relative error of at most 0.015.
Values may be sent and summed in bfloat16 or wider, within the bound.
A program may use at most 64 MiB of HBM per device.

```python
import math
import jax
import jax.numpy as jnp
from jax import lax

D = 2048
W = 1024
FF = 4096
KERNEL = 3
ROWS_B = 256
EXPERTS = 8
FF_PART = 1024
TOK_A = 16384
TOK_B = 2048
CAP = 128
N_TP = 4


def draw_token_rows(key, part):
    base_key, row_key, col_key = jax.random.split(key, 3)
    ramp = jnp.arange(D, dtype=jnp.float32) / D
    base = jnp.clip(jax.random.normal(base_key, (TOK_B, D), jnp.float32), -6.0, 6.0)
    row_scales = jnp.exp(jax.random.uniform(row_key, (TOK_B, 1), jnp.float32, 0.0, math.log(10.0)))
    col_scales = jnp.exp(math.log(10.0) * ramp) * jnp.exp(jax.random.uniform(col_key, (D,), jnp.float32, -0.4, 0.4))
    return (base * row_scales * col_scales[None, :]).astype(jnp.bfloat16)


def draw_routes(key, part):
    blocks = TOK_B // ROWS_B
    capacity = 4 * ROWS_B // EXPERTS
    spare = 2 * ROWS_B - capacity
    hottest = jax.random.randint(jax.random.fold_in(key, 7), (), 0, EXPERTS).astype(jnp.int32)
    ladder = jnp.arange(EXPERTS - 1, dtype=jnp.int32)
    weight_cum = (ladder + 1) * (ladder + 2) // 2
    weight_total = (EXPERTS - 1) * EXPERTS // 2
    run_ends = capacity + spare * weight_cum // weight_total
    position = jnp.arange(2 * ROWS_B, dtype=jnp.int32)
    which_run = jnp.sum((position[:, None] >= run_ends[None, :]).astype(jnp.int32), axis=1)
    which_run = jnp.minimum(which_run, EXPERTS - 2)

    def one_block(block_index):
        block_key = jax.random.fold_in(key, block_index + 11)
        order = jax.random.permutation(jax.random.fold_in(block_key, 1), EXPERTS - 1).astype(jnp.int32)
        others = (hottest + 1 + order) % EXPERTS
        listing = jnp.where(position < capacity, hottest, others[which_run])
        pairs = jnp.stack([listing[:ROWS_B], listing[ROWS_B:]], axis=1)
        shuffle = jax.random.permutation(jax.random.fold_in(block_key, 2), ROWS_B)
        return pairs[shuffle]
    table = jax.vmap(one_block)(jnp.arange(blocks, dtype=jnp.int32))
    return table.reshape(TOK_B, 2).astype(jnp.int32)


def spiked(drawn, rng, source, target, shards_of, factor):
    owner, partner = [(jnp.arange(drawn.shape[axis_at]) // (drawn.shape[axis_at] // shards_of)).reshape([-1 if axis == axis_at else 1 for axis in range(drawn.ndim)]) for axis_at in (source, target)]
    chosen = jax.random.permutation(rng, shards_of)[partner]
    strong = (owner == chosen) | (owner == (partner + shards_of // 2) % shards_of)
    return jnp.where(strong, factor * drawn, drawn)


def levels(rng, dims, shards, least, largest):
    def one(dim, blocks):
        heights = jax.random.uniform(jax.random.fold_in(jax.random.fold_in(rng, 6), dim), (blocks,), jnp.float32, least / len(shards), largest / len(shards))
        return jnp.repeat(jnp.exp(heights), dims[dim] // blocks).reshape((-1,) + (1,) * (len(dims) - dim - 1))

    factor_of = one(*shards[0])
    for cut in shards[1:]:
        factor_of = factor_of * one(*cut)
    return factor_of


def bell_draw(key, extent, scale, limit, pieces=(), kind=jnp.bfloat16):
    result = jax.random.normal(key, extent, jnp.float32) * scale
    if len(pieces) > 0:
        result = levels(key, extent, pieces, -0.22, 0.18) * result
    return jnp.clip(result, min=-limit, max=limit).astype(kind)


def noise_with(rng, shape, width, bound, cuts, heavy, held_as=jnp.bfloat16):
    drawn = width * jax.random.normal(rng, shape, jnp.float32)
    if cuts:
        drawn = drawn * levels(rng, shape, cuts, -0.22, 0.18)
    return jnp.clip(spiked(drawn, jax.random.fold_in(rng, 3), *heavy), -bound, bound).astype(held_as)


def setup_inputs(seed: int = 0) -> dict:
    seeds = jax.random.split(jax.random.key(seed), 12)
    return {
        "conv_input": bell_draw(seeds[0], (W, TOK_A), 1.0, 6.0, ((0, 4), (1, 8))),
        "out_gate": bell_draw(seeds[1], (W, TOK_A), 1.0, 6.0, ((0, 4), (1, 8))),
        "in_gate": bell_draw(seeds[2], (W, TOK_A), 1.0, 6.0, ((0, 4), (1, 8))),
        "conv_taps": bell_draw(seeds[3], (KERNEL, W), 0.6, 3.5, (), jnp.float32),
        "mixer_proj": bell_draw(seeds[4], (W, D), W ** -0.5, 0.1875, ((1, 4),)),
        "token_rows": draw_token_rows(jax.random.fold_in(seeds[11], 71), 0),
        "routes": draw_routes(jax.random.fold_in(seeds[11], 71), 0),
        "route_weights": jnp.clip(0.3 + 0.7 * jax.random.uniform(seeds[7], (TOK_B, 2), jnp.float32) ** levels(seeds[7], (TOK_B, 2), ((0, 8),), -0.2, 0.2), 0.3, 1.0),
        "expert_gate": bell_draw(seeds[8], (EXPERTS, D, FF), D ** -0.5, 0.125, ((0, 8), (2, 4))),
        "expert_up": bell_draw(seeds[9], (EXPERTS, D, FF), D ** -0.5, 0.125, ((0, 8), (2, 4))),
        "expert_down": noise_with(seeds[10], (EXPERTS, FF, D), FF ** -0.5, 0.125, ((0, 8), (1, 4)), (1, 2, 4, 2.0)),
    }


EPSILON = 1e-06

def slot_places(route_ids, capacity, experts):
    flat_ids = route_ids.reshape(-1).astype(jnp.int32)
    hit_table = (flat_ids[:, None] == jnp.arange(experts, dtype=jnp.int32)[None, :]).astype(jnp.int32)
    earlier = jnp.cumsum(hit_table, axis=0) - hit_table
    slot_rank = lax.optimization_barrier(jnp.sum(earlier * hit_table, axis=1))
    return (flat_ids * capacity + slot_rank).astype(jnp.int32)

def mixer(conv_input, out_gate, in_gate, conv_taps, mixer_proj):
    z_rows = (conv_input.astype(jnp.float32) * in_gate.astype(jnp.float32)).astype(jnp.bfloat16)
    length = z_rows.shape[1]
    padded = jnp.pad(z_rows.astype(jnp.float32), ((0, 0), (KERNEL - 1, 0)))
    conv_sum = jnp.zeros(z_rows.shape, jnp.float32)
    for lag_index in range(KERNEL):
        begin = KERNEL - 1 - lag_index
        conv_sum = conv_sum + conv_taps[lag_index][:, None] * padded[:, begin:begin + length]
    gated = (out_gate.astype(jnp.float32) * conv_sum).astype(jnp.bfloat16)
    return jnp.dot(gated.T, mixer_proj, preferred_element_type=jnp.float32).astype(jnp.bfloat16)

def expert_block(inputs):
    rows_in, gate_weight, up_weight, down_weight = inputs
    values = rows_in.astype(jnp.float32)
    row_scale = lax.rsqrt(lax.optimization_barrier(jnp.mean(values * values, axis=1, keepdims=True)) + EPSILON)
    gate_sum = row_scale * jnp.dot(rows_in, gate_weight, preferred_element_type=jnp.float32)
    up_sum = row_scale * jnp.dot(rows_in, up_weight, preferred_element_type=jnp.float32)
    hidden = (jax.nn.silu(gate_sum) * up_sum).astype(jnp.bfloat16)
    split_hidden = hidden.reshape(hidden.shape[0], N_TP, FF_PART).astype(jnp.float32)
    split_down = down_weight.reshape(N_TP, FF_PART, D).astype(jnp.float32)
    partial_value = jnp.einsum('snf,nfd->nsd', split_hidden, split_down).astype(jnp.bfloat16)
    return lax.optimization_barrier(jnp.sum(partial_value.astype(jnp.float32), axis=0)).astype(jnp.bfloat16)

def reference(conv_input, out_gate, in_gate, conv_taps, mixer_proj, token_rows, routes, route_weights, expert_gate, expert_up, expert_down):
    mixed_out = mixer(conv_input, out_gate, in_gate, conv_taps, mixer_proj)
    blocks = TOK_B // ROWS_B
    route_blocks = routes.reshape(blocks, ROWS_B, 2)

    def block_places(route_ids):
        return slot_places(route_ids, CAP, EXPERTS)
    places = jax.vmap(block_places)(route_blocks)
    sources = jnp.arange(2 * ROWS_B, dtype=jnp.int32) // 2

    def fill(rows_in, place_list):
        return jnp.zeros((EXPERTS * CAP, D), jnp.bfloat16).at[place_list].set(rows_in[sources])
    buffers = jax.vmap(fill)(token_rows.reshape(blocks, ROWS_B, D), places)
    by_expert = buffers.reshape(blocks, EXPERTS, CAP, D).transpose(1, 0, 2, 3).reshape(EXPERTS, blocks * CAP, D)
    results = lax.map(expert_block, (by_expert, expert_gate, expert_up, expert_down))
    home = results.reshape(EXPERTS, blocks, CAP, D).transpose(1, 0, 2, 3).reshape(blocks, EXPERTS * CAP, D)

    def pick(rows_in, place_list):
        return rows_in[place_list]
    picked = jax.vmap(pick)(home, places).astype(jnp.float32).reshape(blocks, ROWS_B, 2, D)
    weights = route_weights.reshape(blocks, ROWS_B, 2, 1)
    expert_out = lax.optimization_barrier(jnp.sum(picked * weights, axis=2)).reshape(TOK_B, D).astype(jnp.bfloat16)
    return (mixed_out, expert_out)
```

```python
import jax
import jax.numpy as jnp
from jax import lax
from jax.sharding import PartitionSpec as P

KERNEL = 3
EPSILON = 1e-06
CHUNKS = 2


def passed_along(value, axis, by):
    devices = lax.axis_size(axis)
    pairs = [(i, i + by) for i in range(devices) if 0 <= i + by < devices]
    return lax.ppermute(value, axis, pairs)


def rotated(value, by):
    devices = lax.axis_size("ep")
    return lax.ppermute(value, "ep", [(i, (i + by) % devices) for i in range(devices)])


def swapped(value, bit):
    devices = lax.axis_size("tp")
    return lax.ppermute(value, "tp", [(i, i ^ bit) for i in range(devices)])


def near_order(value, axis, here):
    size = value.shape[axis] // 4
    return [lax.dynamic_slice_in_dim(value, (here ^ bit) * size, size, axis) for bit in range(4)]


def routing(route_ids, capacity, experts):
    rows = route_ids.shape[0]
    names = jnp.arange(experts, dtype=jnp.int32)[None, :]
    hits = [(route_ids[:, k][:, None] == names) for k in range(2)]
    both = (hits[0] | hits[1]).astype(jnp.bfloat16)
    index = jnp.arange(rows, dtype=jnp.int32)
    lower = (index[:, None] > index[None, :]).astype(jnp.bfloat16)
    earlier = jnp.dot(lower, both, preferred_element_type=jnp.float32)
    away = lax.rem(route_ids - lax.axis_index("ep") + experts, experts)
    places = []
    for k in range(2):
        rank = jnp.sum(jnp.where(hits[k], earlier, 0.0), axis=1).astype(jnp.int32)
        places.append(away[:, k] * capacity + rank)
    return places


def expert_hidden(part_in, row_scale, gate_weight, up_weight):
    gate_sum = jnp.dot(part_in, gate_weight, preferred_element_type=jnp.float32)
    up_sum = jnp.dot(part_in, up_weight, preferred_element_type=jnp.float32)
    return (jax.nn.silu(row_scale * gate_sum) * (row_scale * up_sum)).astype(jnp.bfloat16)


def product(hidden, down):
    return jnp.dot(hidden, down, preferred_element_type=jnp.float32).astype(jnp.bfloat16)


def added(one, other):
    return (one.astype(jnp.float32) + other.astype(jnp.float32)).astype(jnp.bfloat16)


def body(
    conv_input,
    out_gate,
    in_gate,
    conv_taps,
    mixer_proj,
    token_rows,
    routes,
    route_weights,
    expert_gate,
    expert_up,
    expert_down,
):
    tp = lax.axis_size("tp")
    here = lax.axis_index("tp")
    square = tp == 4
    width_part = conv_input.shape[0]
    length = conv_input.shape[1]
    local_taps = lax.dynamic_slice_in_dim(conv_taps, here * width_part, width_part, 1)

    experts = lax.axis_size("ep")
    rows_b, cols_part = token_rows.shape
    capacity = 4 * rows_b // experts
    slot_total = experts * capacity
    feature_count = cols_part * tp
    places = routing(routes, capacity, experts)
    slots = jnp.arange(slot_total, dtype=jnp.int32)
    picks = [(slots[:, None] == places[k][None, :]) for k in range(2)]
    chosen = (picks[0] | picks[1]).astype(jnp.bfloat16)
    buffer = jnp.dot(chosen, token_rows, preferred_element_type=jnp.float32).astype(jnp.bfloat16)

    z_rows = (conv_input.astype(jnp.float32) * in_gate.astype(jnp.float32)).astype(jnp.bfloat16)
    rim_rows = passed_along(z_rows[:, length - (KERNEL - 1) :], "ep", 1)
    longer = jnp.concatenate([rim_rows, z_rows], axis=1).astype(jnp.float32)
    conv_sum = jnp.zeros(z_rows.shape, jnp.float32)
    for lag_index in range(KERNEL):
        begin = KERNEL - 1 - lag_index
        conv_sum = conv_sum + local_taps[lag_index][:, None] * longer[:, begin : begin + length]
    gated = (out_gate.astype(jnp.float32) * conv_sum).astype(jnp.bfloat16)

    arrived = [
        rotated(buffer[d * capacity : (d + 1) * capacity], d) if d else buffer[:capacity]
        for d in range(experts)
    ]
    chunk_parts = experts // CHUNKS
    chunks = [
        jnp.concatenate(arrived[c * chunk_parts : (c + 1) * chunk_parts], axis=0)
        for c in range(CHUNKS)
    ]
    gate_weight, up_weight, down_weight = expert_gate[0], expert_up[0], expert_down[0]

    def scale_of(part_in):
        squares = jnp.sum(jnp.square(part_in.astype(jnp.float32)), axis=1)
        return lax.rsqrt(squares / feature_count + EPSILON)[:, None]

    outs = []
    if square:
        gate_weight = jnp.concatenate(near_order(gate_weight, 0, here), axis=0)
        up_weight = jnp.concatenate(near_order(up_weight, 0, here), axis=0)
        proj = jnp.concatenate(near_order(mixer_proj, 0, here), axis=0)
        down = near_order(down_weight, 1, here)
        mix_x, mix_y = swapped(gated, 1), swapped(gated, 2)
        mix_x, mix_y, *chunks = lax.optimization_barrier((mix_x, mix_y, *chunks))
        half = width_part // 2
        mix_far = [swapped(mix_y[:half], 1), swapped(mix_x[half:], 2)]
        for c in range(CHUNKS):
            own = chunks[c]
            by_x, by_y = swapped(own, 1), swapped(own, 2)
            middle = own.shape[0] // 2
            far = jnp.concatenate(
                [swapped(by_y[:middle], 1), swapped(by_x[middle:], 2)], axis=0
            )
            part_in = jnp.concatenate([own, by_x, by_y, far], axis=1)
            hidden = expert_hidden(part_in, scale_of(part_in), gate_weight, up_weight)
            first, second = ((1, 2), (2, 1))[c % 2]
            away = product(hidden, jnp.concatenate([down[first], down[3]], axis=1))
            near = product(hidden, jnp.concatenate([down[0], down[second]], axis=1))
            half_sum = added(near, swapped(away, first))
            outs.append(
                added(half_sum[:, :cols_part], swapped(half_sum[:, cols_part:], second))
            )
        *mix_far, outs[-1] = lax.optimization_barrier((*mix_far, outs[-1]))
        mixer_in = jnp.concatenate([gated, mix_x, mix_y, *mix_far], axis=0)
    else:
        proj = mixer_proj
        mixer_in = lax.all_gather(gated, "tp", axis=0, tiled=True)
        for own in chunks:
            part_in = lax.all_gather(own, "tp", axis=1, tiled=True)
            hidden = expert_hidden(part_in, scale_of(part_in), gate_weight, up_weight)
            outs.append(
                lax.psum_scatter(
                    product(hidden, down_weight), "tp", scatter_dimension=1, tiled=True
                )
            )

    returned = []
    for c in range(CHUNKS):
        for i in range(chunk_parts):
            d = c * chunk_parts + i
            block = outs[c][i * capacity : (i + 1) * capacity]
            returned.append(rotated(block, -d) if d else block)
    returned = jnp.concatenate(returned, axis=0)
    weights = sum(
        jnp.where(slots[None, :] == places[k][:, None], route_weights[:, k][:, None], 0.0)
        for k in range(2)
    )
    high = weights.astype(jnp.bfloat16)
    low = (weights - high.astype(jnp.float32)).astype(jnp.bfloat16)
    both = jnp.dot(
        jnp.concatenate([high, low], axis=0), returned, preferred_element_type=jnp.float32
    )
    expert_out = (both[:rows_b] + both[rows_b:]).astype(jnp.bfloat16)

    mixed_out = lax.dot_general(
        mixer_in, proj, (((0,), (0,)), ((), ())), preferred_element_type=jnp.float32
    ).astype(jnp.bfloat16)
    return (mixed_out, expert_out)


def solution(mesh):
    return jax.shard_map(
        body,
        mesh=mesh,
        in_specs=(
            P("tp", "ep"),
            P("tp", "ep"),
            P("tp", "ep"),
            P(),
            P(None, "tp"),
            P("ep", "tp"),
            P("ep", None),
            P("ep", None),
            P("ep", None, "tp"),
            P("ep", None, "tp"),
            P("ep", "tp", None),
        ),
        out_specs=(P("ep", "tp"), P("ep", "tp")),
        check_vma=False,
    )
```

```python
import jax
import jax.numpy as jnp
from jax import lax
from jax.sharding import PartitionSpec as P

KERNEL = 3
EPSILON = 1e-06
CHUNKS = 2


def passed_along(value, axis, by):
    devices = lax.axis_size(axis)
    pairs = [(i, i + by) for i in range(devices) if 0 <= i + by < devices]
    return lax.ppermute(value, axis, pairs)


def rotated(value, by):
    devices = lax.axis_size("ep")
    return lax.ppermute(value, "ep", [(i, (i + by) % devices) for i in range(devices)])


def swapped(value, bit):
    devices = lax.axis_size("tp")
    return lax.ppermute(value, "tp", [(i, i ^ bit) for i in range(devices)])


def near_order(value, axis, here):
    size = value.shape[axis] // 4
    return [lax.dynamic_slice_in_dim(value, (here ^ bit) * size, size, axis) for bit in range(4)]


def routing(route_ids, capacity, experts):
    rows = route_ids.shape[0]
    names = jnp.arange(experts, dtype=jnp.int32)[None, :]
    hits = [(route_ids[:, k][:, None] == names) for k in range(2)]
    both = (hits[0] | hits[1]).astype(jnp.bfloat16)
    index = jnp.arange(rows, dtype=jnp.int32)
    lower = (index[:, None] > index[None, :]).astype(jnp.bfloat16)
    earlier = jnp.dot(lower, both, preferred_element_type=jnp.float32)
    away = lax.rem(route_ids - lax.axis_index("ep") + experts, experts)
    places = []
    for k in range(2):
        rank = jnp.sum(jnp.where(hits[k], earlier, 0.0), axis=1).astype(jnp.int32)
        places.append(away[:, k] * capacity + rank)
    return places


def expert_hidden(part_in, row_scale, gate_weight, up_weight):
    gate_sum = jnp.dot(part_in, gate_weight, preferred_element_type=jnp.float32)
    up_sum = jnp.dot(part_in, up_weight, preferred_element_type=jnp.float32)
    return (jax.nn.silu(row_scale * gate_sum) * (row_scale * up_sum)).astype(jnp.bfloat16)


def product(hidden, down):
    return jnp.dot(hidden, down, preferred_element_type=jnp.float32).astype(jnp.bfloat16)


def added(one, other):
    return (one.astype(jnp.float32) + other.astype(jnp.float32)).astype(jnp.bfloat16)


def body(
    conv_input,
    out_gate,
    in_gate,
    conv_taps,
    mixer_proj,
    token_rows,
    routes,
    route_weights,
    expert_gate,
    expert_up,
    expert_down,
):
    tp = lax.axis_size("tp")
    here = lax.axis_index("tp")
    square = tp == 4
    width_part = conv_input.shape[0]
    length = conv_input.shape[1]
    local_taps = lax.dynamic_slice_in_dim(conv_taps, here * width_part, width_part, 1)

    experts = lax.axis_size("ep")
    rows_b, cols_part = token_rows.shape
    capacity = 4 * rows_b // experts
    slot_total = experts * capacity
    feature_count = cols_part * tp
    places = routing(routes, capacity, experts)
    slots = jnp.arange(slot_total, dtype=jnp.int32)
    picks = [(slots[:, None] == places[k][None, :]) for k in range(2)]
    chosen = (picks[0] | picks[1]).astype(jnp.bfloat16)
    buffer = jnp.dot(chosen, token_rows, preferred_element_type=jnp.float32).astype(jnp.bfloat16)

    z_rows = (conv_input.astype(jnp.float32) * in_gate.astype(jnp.float32)).astype(jnp.bfloat16)
    rim_rows = passed_along(z_rows[:, length - (KERNEL - 1) :], "ep", 1)
    longer = jnp.concatenate([rim_rows, z_rows], axis=1).astype(jnp.float32)
    conv_sum = jnp.zeros(z_rows.shape, jnp.float32)
    for lag_index in range(KERNEL):
        begin = KERNEL - 1 - lag_index
        conv_sum = conv_sum + local_taps[lag_index][:, None] * longer[:, begin : begin + length]
    gated = (out_gate.astype(jnp.float32) * conv_sum).astype(jnp.bfloat16)

    gated, buffer = lax.optimization_barrier((gated, buffer))
    arrived = [
        rotated(buffer[d * capacity : (d + 1) * capacity], d) if d else buffer[:capacity]
        for d in range(experts)
    ]
    chunk_parts = experts // CHUNKS
    chunks = [
        jnp.concatenate(arrived[c * chunk_parts : (c + 1) * chunk_parts], axis=0)
        for c in range(CHUNKS)
    ]
    gate_weight, up_weight, down_weight = expert_gate[0], expert_up[0], expert_down[0]

    def squares_of(part_in):
        return jnp.sum(jnp.square(part_in.astype(jnp.float32)), axis=1)

    def scale_of(squares):
        return lax.rsqrt(squares / feature_count + EPSILON)[:, None]

    outs, returned = [], []

    def send_back(c):
        for i in range(chunk_parts):
            d = c * chunk_parts + i
            block = outs[c][i * capacity : (i + 1) * capacity]
            returned.append(rotated(block, -d) if d else block)

    if square:
        chunks[0], gate_weight, up_weight, down_weight, mixer_proj = lax.optimization_barrier(
            (chunks[0], gate_weight, up_weight, down_weight, mixer_proj)
        )
        weights_in = (
            jnp.concatenate(near_order(gate_weight, 0, here), axis=0),
            jnp.concatenate(near_order(up_weight, 0, here), axis=0),
            *near_order(down_weight, 1, here),
        )
        proj = jnp.concatenate(near_order(mixer_proj, 0, here), axis=0)
        mix_x, mix_y = swapped(gated, 1), swapped(gated, 2)
        mix_x, mix_y, chunks[0] = lax.optimization_barrier((mix_x, mix_y, chunks[0]))
        half = width_part // 2
        mix_far = (mix_y[:half], mix_x[half:])
        for c in range(CHUNKS):
            own = chunks[c]
            by_x, by_y = swapped(own, 1), swapped(own, 2)
            middle = own.shape[0] // 2
            far = (by_y[:middle], by_x[middle:])
            if c == 0:
                by_x, by_y, far, weights_in = lax.optimization_barrier(
                    (by_x, by_y, far, weights_in)
                )
            gate_weight, up_weight, *down = weights_in
            squares = squares_of(own) + squares_of(by_x) + squares_of(by_y)
            squares, *far = lax.optimization_barrier((squares, *far)) if c else (squares, *far)
            far = [swapped(far[0], 1), swapped(far[1], 2)]
            if c == 0:
                far, chunks[1:] = lax.optimization_barrier((far, chunks[1:]))
            far = jnp.concatenate(far, axis=0)
            squares = squares + squares_of(far)
            part_in = jnp.concatenate([own, by_x, by_y, far], axis=1)
            hidden = expert_hidden(part_in, scale_of(squares), gate_weight, up_weight)
            sums = []
            for first, second, rows in ((1, 2, hidden[:middle]), (2, 1, hidden[middle:])):
                away = product(rows, jnp.concatenate([down[first], down[3]], axis=1))
                near = product(rows, jnp.concatenate([down[0], down[second]], axis=1))
                both = added(near, swapped(away, first))
                sums.append((both[:, :cols_part], both[:, cols_part:], second))
            if c == 0:
                kept = [part[:2] for part in sums]
                kept, mix_far = lax.optimization_barrier((kept, mix_far))
                sums = [(*pair, part[2]) for pair, part in zip(kept, sums)]
                mix_far = [swapped(mix_far[0], 1), swapped(mix_far[1], 2)]
            outs.append(
                jnp.concatenate(
                    [added(keep, swapped(send, second)) for keep, send, second in sums], axis=0
                )
            )
            if c == CHUNKS - 1:
                returned, mix_far, outs[c] = lax.optimization_barrier(
                    (returned, mix_far, outs[c])
                )
            send_back(c)
        mixer_in = jnp.concatenate([gated, mix_x, mix_y, *mix_far], axis=0)
    else:
        proj = mixer_proj
        mixer_in = lax.all_gather(gated, "tp", axis=0, tiled=True)
        for c, own in enumerate(chunks):
            part_in = lax.all_gather(own, "tp", axis=1, tiled=True)
            hidden = expert_hidden(part_in, scale_of(squares_of(part_in)), gate_weight, up_weight)
            outs.append(
                lax.psum_scatter(
                    product(hidden, down_weight), "tp", scatter_dimension=1, tiled=True
                )
            )
            send_back(c)

    returned = jnp.concatenate(returned, axis=0)
    weights = sum(
        jnp.where(slots[None, :] == places[k][:, None], route_weights[:, k][:, None], 0.0)
        for k in range(2)
    )
    high = weights.astype(jnp.bfloat16)
    low = (weights - high.astype(jnp.float32)).astype(jnp.bfloat16)
    both = jnp.dot(
        jnp.concatenate([high, low], axis=0), returned, preferred_element_type=jnp.float32
    )
    expert_out = (both[:rows_b] + both[rows_b:]).astype(jnp.bfloat16)

    mixed_out = lax.dot_general(
        mixer_in, proj, (((0,), (0,)), ((), ())), preferred_element_type=jnp.float32
    ).astype(jnp.bfloat16)
    return (mixed_out, expert_out)


def solution(mesh):
    return jax.shard_map(
        body,
        mesh=mesh,
        in_specs=(
            P("tp", "ep"),
            P("tp", "ep"),
            P("tp", "ep"),
            P(),
            P(None, "tp"),
            P("ep", "tp"),
            P("ep", None),
            P("ep", None),
            P("ep", None, "tp"),
            P("ep", None, "tp"),
            P("ep", "tp", None),
        ),
        out_specs=(P("ep", "tp"), P("ep", "tp")),
        check_vma=False,
    )
```
